32 devices in a mesh: fs: 16 (over z, y, x), tp: 2 (over core).
Axes of the slice: x: 2, y: 2, z: 4, core: 2. Of those that a mesh axis runs over, the one named last changes fastest.
Arguments:
- tokens: bfloat16 [12288, 2048], P('fs'), may hold values from -6 to 6
- norm_gain: float32 [2048], replicated, may hold values from 0.1 to 1.9
- up_weight: float32 [2048, 8192], P('fs', 'tp'), may hold values from -0.125 to 0.125
- up_scale: float32 [8192], P('tp'), may hold values from 0.5 to 2
- down_weight: float32 [8192, 2048], P('tp', 'fs'), may hold values from -0.09375 to 0.09375
- down_scale: float32 [1, 2048], replicated, may hold values from 0.5 to 2
Outputs:
- mixed: bfloat16 [12288, 2048], P('fs', 'tp')
The draws below stay inside these ranges and needn't reach their ends.
All inputs are finite; a program needn't handle non-finite values.
Results may differ from the reference program's by a relative error of at most 0.014.
Values may be sent and summed in bfloat16 or wider, within the bound.
No kernel may reach another device: no remote copies, remote signals or barrier semaphores. Data moves between devices by JAX's collectives and lax.ppermute only.
A program may use at most 128 MiB of HBM per device.

```python
import math
import jax
import jax.numpy as jnp
from jax import lax

D = 2048
FF = 8192
TOKENS = 12288
N_FS = 16
N_TP = 2


def with_spikes(drawn, stream_key, source, target, shards_of, factor):
    def block_of(axis_at):
        return (jnp.arange(drawn.shape[axis_at]) // (drawn.shape[axis_at] // shards_of)).reshape((-1,) + (1,) * (drawn.ndim - 1 - axis_at))

    near = jax.random.permutation(stream_key, shards_of)[block_of(target)]
    far = (block_of(target) + shards_of // 2) % shards_of
    return jnp.where((block_of(source) == near) | (block_of(source) == far), factor * drawn, drawn)


def level_of(key, extent, cuts, low, high):
    level = 1.0
    for dim, shards_of in cuts:
        draws = jax.random.uniform(jax.random.fold_in(jax.random.fold_in(key, 6), dim), (shards_of,), jnp.float32, low / len(cuts), high / len(cuts))
        level = level * jnp.repeat(jnp.exp(draws), extent[dim] // shards_of).reshape((-1,) + (1,) * (len(extent) - 1 - dim))
    return level


def bell_draw(stream_key, extent, deviation, bound, shards=(), dtype=jnp.bfloat16):
    factor_of = level_of(stream_key, extent, shards, -0.22, 0.18) if shards else 1.0
    drawn = jax.random.normal(stream_key, extent, jnp.float32) * deviation * factor_of
    return jnp.minimum(jnp.maximum(drawn, -bound), bound).astype(dtype)


def gaussian_with(key, shape, spread, most, pieces, heavy, held_as=jnp.bfloat16):
    drawn = spread * jax.random.normal(key, shape, jnp.float32)
    if pieces:
        drawn = drawn * level_of(key, shape, pieces, -0.22, 0.18)
    return jnp.clip(with_spikes(drawn, jax.random.fold_in(key, 3), *heavy), -most, most).astype(held_as)


def setup_inputs(seed: int = 0) -> dict:
    arg_keys = jax.random.split(jax.random.key(seed), 7)
    tokens = bell_draw(arg_keys[0], (TOKENS, D), 1.0, 6.0, ((0, 16),))
    norm_gain = jnp.clip(1.0 + 0.18 * jax.random.normal(arg_keys[1], (D,), jnp.float32), 0.1, 1.9)
    up_weight = bell_draw(arg_keys[2], (D, FF), D ** -0.5, 0.125, ((0, 16), (1, 2)), jnp.float32)
    up_scale = jnp.clip(jnp.exp(math.log(2.0) - 1.3862944 * jax.random.uniform(arg_keys[3], (FF,), jnp.float32) ** level_of(arg_keys[3], (FF,), ((0, 2),), -0.2, 0.2)), 0.5, 2.0)
    down_weight = gaussian_with(arg_keys[4], (FF, D), FF ** -0.5, 0.09375, ((0, 2), (1, 16)), (0, 1, 16, 2.0), jnp.float32)
    down_scale = jnp.clip(jnp.exp(jax.random.uniform(arg_keys[5], (1, D), jnp.float32, math.log(0.5), math.log(2.0))), 0.5, 2.0)
    return dict(tokens=tokens, norm_gain=norm_gain, up_weight=up_weight, up_scale=up_scale, down_weight=down_weight, down_scale=down_scale)


def reference(tokens, norm_gain, up_weight, up_scale, down_weight, down_scale):
    up_cast = up_weight.astype(jnp.bfloat16)
    down_cast = down_weight.astype(jnp.bfloat16)
    block_ff = FF // N_TP
    groups = tokens.reshape(N_FS, TOKENS // N_FS, D)

    def one_group(rows):
        values = rows.astype(jnp.float32)
        normed = (values * lax.rsqrt(lax.optimization_barrier(jnp.mean(values * values, axis=-1, keepdims=True)) + 1e-06) * norm_gain).astype(jnp.bfloat16)
        pre = jnp.dot(normed, up_cast, preferred_element_type=jnp.float32) * up_scale
        hidden = jnp.square(jnp.maximum(pre, 0.0)).astype(jnp.bfloat16)
        total = jnp.zeros((rows.shape[0], D), jnp.float32)
        for block in range(N_TP):
            lower = block * block_ff
            partial_value = jnp.dot(hidden[:, lower:lower + block_ff], down_cast[lower:lower + block_ff, :], preferred_element_type=jnp.float32) * down_scale
            total = total + partial_value.astype(jnp.bfloat16).astype(jnp.float32)
        return total.astype(jnp.bfloat16)
    return lax.map(one_group, groups).reshape(TOKENS, D)
```

```python
import functools

import jax
import jax.numpy as jnp
from jax import lax
from jax.experimental import pallas as pl
from jax.experimental.pallas import tpu as pltpu
from jax.sharding import PartitionSpec as P

EPS = 1e-06
LANES = 128


def normalize(tokens, norm_gain):
    values = tokens.astype(jnp.float32)
    return (
        values * lax.rsqrt(jnp.mean(values * values, axis=-1, keepdims=True) + EPS) * norm_gain
    ).astype(jnp.bfloat16)


def gather_plan(tokens, norm_gain, up_weight, up_scale, down_weight, down_scale):
    normed = normalize(tokens, norm_gain)
    up_full = lax.all_gather(up_weight.astype(jnp.bfloat16), "fs", axis=0, tiled=True)
    pre = jnp.dot(normed, up_full, preferred_element_type=jnp.float32) * up_scale
    hidden = jnp.square(jnp.maximum(pre, 0.0)).astype(jnp.bfloat16)
    down_full = lax.all_gather(down_weight.astype(jnp.bfloat16), "fs", axis=1, tiled=True)
    partial_value = jnp.dot(hidden, down_full, preferred_element_type=jnp.float32) * down_scale
    rounded = partial_value.astype(jnp.bfloat16)
    return (
        lax.psum_scatter(rounded, "tp", scatter_dimension=1, tiled=True)
        .astype(jnp.float32)
        .astype(jnp.bfloat16)
    )


def matmul_kernel(rows_axis, squared, n_tile, offsets, lhs, scale, *refs):
    blocks, (out, w, sems) = refs[:-3], refs[-3:]

    @pl.when(pl.program_id(0) == 0)
    def _():
        copies = []
        for at, block in enumerate(blocks):
            where = pl.ds(pl.multiple_of(offsets[at], LANES), block.shape[rows_axis])
            target = w.at[where, :] if rows_axis == 0 else w.at[:, where]
            copies.append(pltpu.make_async_copy(block, target, sems.at[at]))
        for copy in copies:
            copy.start()
        for copy in copies:
            copy.wait()

    def step(at, carry):
        where = pl.ds(pl.multiple_of(at * n_tile, LANES), n_tile)
        value = jnp.dot(lhs[...], w[:, where], preferred_element_type=jnp.float32) * scale[:, where]
        if squared:
            value = jnp.square(jnp.maximum(value, 0.0))
        out[:, where] = value.astype(out.dtype)
        return carry

    lax.fori_loop(0, w.shape[1] // n_tile, step, 0)


def matmul(lhs, blocks, offsets, scale, rows_axis, squared, m_tile, n_tile):
    m, depth = lhs.shape
    n = scale.shape[1]
    count = len(blocks)
    return pl.pallas_call(
        functools.partial(matmul_kernel, rows_axis, squared, n_tile),
        grid_spec=pltpu.PrefetchScalarGridSpec(
            num_scalar_prefetch=1,
            grid=(m // m_tile,),
            in_specs=[
                pl.BlockSpec((m_tile, depth), lambda i, s: (i, 0)),
                pl.BlockSpec((1, n), lambda i, s: (0, 0)),
            ]
            + [pl.BlockSpec(memory_space=pl.ANY)] * count,
            out_specs=pl.BlockSpec((m_tile, n), lambda i, s: (i, 0)),
            scratch_shapes=[pltpu.VMEM((depth, n), jnp.bfloat16), pltpu.SemaphoreType.DMA((count,))],
        ),
        out_shape=jax.ShapeDtypeStruct((m, n), jnp.bfloat16),
        compiler_params=pltpu.CompilerParams(
            dimension_semantics=("arbitrary",), vmem_limit_bytes=32 * 1024 * 1024
        ),
        cost_estimate=pl.CostEstimate(
            flops=2 * m * depth * n,
            bytes_accessed=2 * (m * depth + depth * n + m * n),
            transcendentals=0,
        ),
        name="up_mm" if squared else "down_mm",
    )(offsets, lhs, scale, *blocks)


def paired_plan(grid, tokens, norm_gain, up_weight, up_scale, down_weight, down_scale):
    nz, ny, nx = grid
    chips = nz * ny * nx
    me, t = lax.axis_index("fs"), lax.axis_index("tp")
    z, y, x = me // (ny * nx), me // nx % ny, me % nx
    part = z % 2
    rows, width = tokens.shape
    hidden_half = up_weight.shape[1] // 2
    block = up_weight.shape[0]

    def pairs(dz, dy, dx):
        out = []
        for c in range(chips):
            cz, cy, cx = c // (ny * nx), c // nx % ny, c % nx
            out.append((c, ((cz ^ dz) * ny + (cy ^ dy)) * nx + (cx ^ dx)))
        return out

    def hop(value, dz, dy, dx):
        return lax.ppermute(value, "fs", pairs(dz, dy, dx))

    def across(value):
        return lax.ppermute(value, "tp", [(0, 1), (1, 0)])

    def spread(same, other):
        got = {(0, 0, 0): same}
        for k in range(1, nz):
            got[k, 0, 0] = hop(same if k % 2 == 0 else other, k, 0, 0)
        for k in range(nz):
            got[k, 0, 1] = hop(got[k, 0, 0], 0, 0, 1)
            got[k, 1, 0] = hop(got[k, 0, 0], 0, 1, 0)
            got[k, 1, 1] = hop(got[k, 0, 1], 0, 1, 0) if k % 2 == 0 else hop(got[k, 1, 0], 0, 0, 1)
        return got

    places = [(k, j, i) for k in range(nz) for j in range(ny) for i in range(nx)]

    def slot(k, j, i):
        return ((z ^ k) * ny + (y ^ j)) * nx + (x ^ i)

    up_same = lax.dynamic_slice(up_weight, (0, part * hidden_half), (block, hidden_half)).astype(jnp.bfloat16)
    up_other = lax.dynamic_slice(up_weight, (0, (1 - part) * hidden_half), (block, hidden_half)).astype(jnp.bfloat16)
    up = spread(up_same, up_other)

    own = normalize(tokens, norm_gain)
    half = rows // 2
    got_half = hop(lax.dynamic_slice(own, (t * half, 0), (half, width)), 1, 0, 0)
    peer_half = across(got_half)
    partner = jnp.where(
        t == 0,
        jnp.concatenate([got_half, peer_half], 0),
        jnp.concatenate([peer_half, got_half], 0),
    )

    down_same = lax.dynamic_slice(down_weight, (part * hidden_half, 0), (hidden_half, block)).astype(jnp.bfloat16)
    down_other = lax.dynamic_slice(down_weight, ((1 - part) * hidden_half, 0), (hidden_half, block)).astype(jnp.bfloat16)
    down = spread(down_same, down_other)

    scale_up = lax.dynamic_slice(up_scale, (part * hidden_half,), (hidden_half,))[None, :]
    up_offsets = jnp.stack([slot(*place) * block for place in places]).astype(jnp.int32)
    up_blocks = [up[place] for place in places]
    hidden_own, hidden_partner = (
        matmul(lhs, up_blocks, up_offsets, scale_up, 0, True, rows // 2, 256) for lhs in (own, partner)
    )

    group = ny * nx * block
    down_offsets = jnp.stack([(slot(0, j, i) % (ny * nx)) * block for j in range(ny) for i in range(nx)]).astype(jnp.int32)
    owner = lambda cz, k: (cz ^ k) // (nz // 2)
    kept, arrived = [], []
    for k in range(nz):
        blocks = [down[k, j, i] for j in range(ny) for i in range(nx)]
        scale = lax.dynamic_slice(down_scale, (0, (z ^ k) * group), (1, group))
        swap = []
        send = []
        for c in range(chips):
            cz = c // (ny * nx)
            h = owner(cz, k)
            swap.append((c * 2 + 1 - h, c * 2 + h))
            send.append((c * 2 + h, (((cz ^ 1) * (ny * nx)) + c % (ny * nx)) * 2 + h))
        for_partner = matmul(hidden_partner, blocks, down_offsets, scale, 1, False, rows // 2, group)
        for_partner = (
            for_partner.astype(jnp.float32) + lax.ppermute(for_partner, ("fs", "tp"), swap).astype(jnp.float32)
        ).astype(jnp.bfloat16)
        arrived.append(lax.ppermute(for_partner, ("fs", "tp"), send))
        for_own = matmul(hidden_own, blocks, down_offsets, scale, 1, False, rows // 2, group)
        kept.append((for_own, lax.ppermute(for_own, ("fs", "tp"), swap)))

    totals = [
        kept[k][0].astype(jnp.float32) + kept[k][1].astype(jnp.float32) + arrived[k ^ 1].astype(jnp.float32)
        for k in range(nz)
    ]
    columns = []
    for e in range(nz // 2):
        k = (t * (nz // 2) + e) ^ z
        columns.append(
            jnp.where(k < 2, jnp.where(k == 0, totals[0], totals[1]), jnp.where(k == 2, totals[2], totals[3]))
        )
    return jnp.concatenate(columns, 1).astype(jnp.bfloat16)


def chip_grid(mesh):
    devices = mesh.devices
    if devices.ndim != 2 or devices.shape[1] != 2:
        return None
    at = [[getattr(d, "coords", None) for d in row] for row in devices]
    if any(c is None for row in at for c in row) or any(tuple(row[0]) != tuple(row[1]) for row in at):
        return None
    at = [tuple(row[0]) for row in at]
    nx, ny, nz = (max(c[d] for c in at) + 1 for d in range(3))
    if (nx, ny, nz) != (2, 2, 4) or len(at) != nx * ny * nz:
        return None
    if any(c != (i % nx, i // nx % ny, i // (nx * ny)) for i, c in enumerate(at)):
        return None
    return nz, ny, nx


def solution(mesh):
    in_specs = (P("fs", None), P(), P("fs", "tp"), P("tp"), P("tp", "fs"), P())
    out_specs = P("fs", "tp")
    grid = chip_grid(mesh)
    body = gather_plan if grid is None else functools.partial(paired_plan, grid)
    return jax.shard_map(body, mesh=mesh, in_specs=in_specs, out_specs=out_specs, check_vma=False)
```
